32 devices in a mesh: ep: 8 (over z, x), tp: 4 (over y, core).
Axes of the slice: x: 2, y: 2, z: 4, core: 2. Of those that a mesh axis runs over, the one named last changes fastest.
Arguments:
- blender_incoming_features: bfloat16 [2048, 4096], P('ep', 'tp'), may hold values from -6 to 6
- entry_latent_matrix: bfloat16 [2048, 2048], P('ep', 'tp'), may hold values from -6 to 6
- exit_latent_matrix: bfloat16 [2048, 2048], P('ep', 'tp'), may hold values from -6 to 6
- unactivated_valve: bfloat16 [2048, 4096], P('ep', 'tp'), may hold values from -6 to 6
- presoftplus_strides: float32 [2048, 64], P('ep', 'tp'), may hold values from -7 to 7
- extra_attenuation: float32 [2048, 64], P('ep', 'tp'), may hold values from -1 to 0
- incoming_feature_kernel: bfloat16 [4, 4096], P(None, 'tp'), may hold values from -3 to 3
- entry_latent_kernel: bfloat16 [4, 2048], P(None, 'tp'), may hold values from -3 to 3
- exit_latent_kernel: bfloat16 [4, 2048], P(None, 'tp'), may hold values from -3 to 3
- stride_offset_vector: float32 [64], P('tp'), may hold values from -1 to 1
- attenuation_speed_exponent: float32 [64], P('tp'), may hold values from -16 to -3
- bypass_coef_vector: float32 [64], P('tp'), may hold values from 0.5 to 4
- cluster_rescale_coefs: bfloat16 [4096], P('tp'), may hold values from 0.099609375 to 1.8984375
- blender_result_matrix: bfloat16 [4096, 2048], P('tp'), may hold values from -0.09375 to 0.09375
- latter_microbatch_activations: bfloat16 [2048, 2048], P('ep'), may hold values from -6 to 6
- specialist_rescale_coefs: bfloat16 [2048], replicated, may hold values from 0.099609375 to 1.8984375
- specialist_valve_matrix: bfloat16 [8, 2048, 4096], P('ep', None, 'tp'), may hold values from -0.125 to 0.125
- specialist_expand_matrix: bfloat16 [8, 2048, 4096], P('ep', None, 'tp'), may hold values from -0.125 to 0.125
- specialist_contract_matrix: bfloat16 [8, 4096, 2048], P('ep', 'tp'), may hold values from -0.125 to 0.125
- specialist_picks: int32 [2048, 2], P('ep'), may hold values from 0 to 7, all different within a row; in each aligned block of 256 rows (0 to 255, 256 to 511, ...) at most 96 rows name the same one
- selected_specialist_coefs: float32 [2048, 2], P('ep'), may hold values from 0.1 to 1
Outputs:
- mixed_a: bfloat16 [2048, 2048], P(('ep', 'tp'))
- mixed_b: bfloat16 [2048, 2048], P('ep', 'tp')
The draws below stay inside these ranges and needn't reach their ends.
Inputs may be any that keep to these rules, and one draw needn't show every extreme that they name: `specialist_picks`: in each aligned block of 256 rows, the rows of one index of ep, no expert is named by more than 96 rows, a bound that some block reaches.
All inputs are finite; a program needn't handle non-finite values.
Results may differ from the reference program's by a relative error of at most 0.019.
Values may be sent and summed in bfloat16 or wider, within the bound.
A program may use at most 64 MiB of HBM per device.

```python
import math
import jax
import jax.numpy as jnp
import numpy as np
from jax import lax

D = 2048
HEADS = 64
HEAD_DIM = 64
SHARING_CLUSTERS = 16
STATE = 128
CONV = 4
BLOCK = 64
FF = 4096
TOPK = 2
TOK_B_DEV = 256
INNER = 4096
EXPERTS = 8
SEQ_A = 2048
TOKENS_B = 2048
CAP = 96
N_EP = 8
N_TP = 4


def draw_presoftplus_strides(key, part):
    base_key, shift_key = jax.random.split(jax.random.fold_in(key, 3))
    base_draw = jnp.clip(jax.random.normal(base_key, (SEQ_A, HEADS), jnp.float32), -6.0, 6.0)
    offsets = jax.random.uniform(shift_key, (SEQ_A // BLOCK, 1), jnp.float32, -0.8, 0.8)
    return base_draw + jnp.repeat(offsets, BLOCK, axis=0)


def draw_attenuation_speed_exponent(key, part):
    pick_key, slow_key, fast_key = jax.random.split(jax.random.fold_in(key, 7), 3)
    slow_share = 50
    is_slow = jax.random.randint(pick_key, (HEADS,), 0, 100) < slow_share
    slow_rates = jax.random.uniform(slow_key, (HEADS,), jnp.float32, math.log(0.05 / SEQ_A), math.log(0.4 / SEQ_A))
    fast_rates = jax.random.uniform(fast_key, (HEADS,), jnp.float32, math.log(0.01), math.log(0.035))
    return jnp.where(is_slow, slow_rates, fast_rates)


def draw_extra_attenuation(key, part):
    place_key, factor_key = jax.random.split(jax.random.fold_in(key, 13))
    word_locations = jax.random.randint(place_key, (2,), 0, SEQ_A)
    multiplier_entries = jax.random.uniform(factor_key, (HEADS,), jnp.float32, math.log(0.55), math.log(0.8))
    line_ordinal_array = jnp.arange(SEQ_A)
    spike_marker = jnp.any(line_ordinal_array[:, None] == word_locations[None, :], axis=1)
    return jnp.where(spike_marker[:, None], multiplier_entries[None, :], jnp.zeros((), jnp.float32))


def spiked(entries, stream_key, source, target, parts, factor):
    owner, partner = [(jnp.arange(entries.shape[position]) // (entries.shape[position] // parts)).reshape([-1 if axis == position else 1 for axis in range(entries.ndim)]) for position in (source, target)]
    chosen = jax.random.permutation(stream_key, parts)[partner]
    strong = (owner == chosen) | (owner == (partner + parts // 2) % parts)
    return jnp.where(strong, factor * entries, entries)


def shard_levels(own_key, dims, cuts, low, high):
    gain, own = 1.0, jax.random.fold_in(own_key, 6)
    for dim, parts in cuts:
        steps = jnp.exp(jax.random.uniform(jax.random.fold_in(own, dim), (parts,), jnp.float32, low / len(cuts), high / len(cuts)))
        gain = gain * jnp.repeat(steps, dims[dim] // parts).reshape([-1 if axis == dim else 1 for axis in range(len(dims))])
    return gain


def assign_block(stream_key, own, number, rows, number_of, top, limit, skew):
    order = jax.random.permutation(stream_key, number_of)
    crowded, common = portions_of(number_of, rows * top, limit, skew, True), portions_of(number_of, rows * top, limit, skew, False)
    places = jnp.arange(number_of)

    def named(tallies, rotation):
        used = int((tallies > 0).sum())
        fixed = max(1, used // 4)
        moved = fixed + (places - fixed + rotation * (used - fixed)) % max(1, number_of - fixed)
        return jnp.zeros((number_of,), jnp.int32).at[order[jnp.where(places < fixed, places, moved)]].set(jnp.asarray(tallies, jnp.int32))

    tallies = jnp.where(number % 4 == 0, named(crowded, number // 4), named(common, number - number // 4 - 1))
    mixed = jax.random.permutation(jax.random.fold_in(own, 3), number_of)
    giver, receiver = mixed[0:number_of // 2 * 2:2], mixed[1:number_of // 2 * 2:2]
    margin = jnp.minimum(tallies[giver] - 1, limit - tallies[receiver]) // 2
    margin = jnp.where((giver == order[0]) | (receiver == order[0]) | (tallies[receiver] == 0), 0, jnp.maximum(margin, 0))
    moved = jax.random.randint(jax.random.fold_in(own, 4), (number_of // 2,), 0, 1 << 20) % (margin + 1)
    tallies = tallies.at[giver].add(-moved).at[receiver].add(moved)
    items = jnp.searchsorted(jnp.cumsum(tallies), jnp.arange(rows * top), side="right").astype(jnp.int32)
    grid = items.reshape(top, rows).T
    grid = grid[jax.random.permutation(jax.random.fold_in(own, 1), rows)]
    rotation = jax.random.randint(jax.random.fold_in(own, 2), (rows, 1), 0, top)
    return jnp.take_along_axis(grid, (jnp.arange(top)[None, :] + rotation) % top, axis=1)


def portions_of(count, total, reach, skew, full):
    portions = [(1 << 20) // math.isqrt(standing ** skew) + 1 for standing in range(1, count + 1)]
    largest = reach if full else min(reach, max(-(-total // count), total * portions[0] // sum(portions)))
    least = 1 if total - largest >= count - 1 else 0
    given, surplus = [largest] + [least] * (count - 1), total - largest - least * (count - 1)
    while surplus > 0:
        movable = [i for i in range(1, count) if given[i] < largest] or [i for i in range(1, count) if given[i] < reach]
        pool, remaining = sum([portions[i] for i in movable]), surplus
        for i in movable:
            extra = min(reach - given[i], max(1, remaining * portions[i] // pool), surplus)
            given[i] = given[i] + extra
            surplus = surplus - extra
    return np.array(given)


def scatter_about(own_key, shape, width, bound, shards=(), held_as=jnp.bfloat16):
    result = jax.random.normal(own_key, shape, jnp.float32) * width
    if len(shards) > 0:
        result = shard_levels(own_key, shape, shards, -0.22, 0.18) * result
    return jnp.clip(result, min=-bound, max=bound).astype(held_as)


def noise_with(key, extent, deviation, limit, cuts, heavy, kind=jnp.bfloat16):
    entries = deviation * jax.random.normal(key, extent, jnp.float32)
    if cuts:
        entries = entries * shard_levels(key, extent, cuts, -0.22, 0.18)
    return jnp.clip(spiked(entries, jax.random.fold_in(key, 3), *heavy), -limit, limit).astype(kind)


def setup_inputs(seed: int = 0) -> dict:
    streams_of = jax.random.split(jax.random.key(seed), 22)
    blender_incoming_features = scatter_about(streams_of[0], (SEQ_A, INNER), 1.0, 6.0, ((0, 8), (1, 4)))
    entry_latent_matrix = scatter_about(streams_of[1], (SEQ_A, SHARING_CLUSTERS * STATE), 1.0, 6.0, ((0, 8), (1, 4)))
    exit_latent_matrix = scatter_about(streams_of[2], (SEQ_A, SHARING_CLUSTERS * STATE), 1.0, 6.0, ((0, 8), (1, 4)))
    unactivated_valve = scatter_about(streams_of[3], (SEQ_A, INNER), 1.0, 6.0, ((0, 8), (1, 4)))
    presoftplus_strides = draw_presoftplus_strides(jax.random.fold_in(streams_of[21], 71), 0)
    extra_attenuation = draw_extra_attenuation(jax.random.fold_in(streams_of[21], 71), 0)
    incoming_feature_kernel = scatter_about(streams_of[6], (CONV, INNER), CONV ** -0.5, 3.0, ((1, 4),))
    entry_latent_kernel = scatter_about(streams_of[7], (CONV, SHARING_CLUSTERS * STATE), CONV ** -0.5, 3.0, ((1, 4),))
    exit_latent_kernel = scatter_about(streams_of[8], (CONV, SHARING_CLUSTERS * STATE), CONV ** -0.5, 3.0, ((1, 4),))
    stride_offset_vector = jnp.clip(jax.random.uniform(streams_of[9], (HEADS,), jnp.float32, -1.0, 1.0) * shard_levels(streams_of[9], (HEADS,), ((0, 4),), -0.4, 0.0), -1.0, 1.0)
    attenuation_speed_exponent = draw_attenuation_speed_exponent(jax.random.fold_in(streams_of[21], 71), 0)
    bypass_coef_vector = jnp.clip(jnp.exp(math.log(4.0) - 2.0794415 * jax.random.uniform(streams_of[11], (HEADS,), jnp.float32) ** shard_levels(streams_of[11], (HEADS,), ((0, 4),), -0.2, 0.2)), 0.5, 4.0)
    cluster_rescale_coefs = jnp.clip(1.0 + 0.18 * jax.random.normal(streams_of[12], (INNER,), jnp.float32), 0.099609375, 1.8984375).astype(jnp.bfloat16)
    blender_result_matrix = scatter_about(streams_of[13], (INNER, D), INNER ** -0.5, 0.09375, ((0, 4),))
    latter_microbatch_activations = scatter_about(streams_of[14], (TOKENS_B, D), 1.0, 6.0, ((0, 8),))
    specialist_rescale_coefs = jnp.clip(1.0 + 0.18 * jax.random.normal(streams_of[15], (D,), jnp.float32), 0.099609375, 1.8984375).astype(jnp.bfloat16)
    specialist_valve_matrix = scatter_about(streams_of[16], (EXPERTS, D, FF), D ** -0.5, 0.125, ((0, 8), (2, 4)))
    specialist_expand_matrix = scatter_about(streams_of[17], (EXPERTS, D, FF), D ** -0.5, 0.125, ((0, 8), (2, 4)))
    specialist_contract_matrix = noise_with(streams_of[18], (EXPERTS, FF, D), FF ** -0.5, 0.125, ((0, 8), (1, 4)), (1, 2, 4, 2.0))
    specialist_picks_keys = jax.random.split(jax.random.fold_in(streams_of[19], 1), TOKENS_B // TOK_B_DEV)
    specialist_picks_turns = jax.random.permutation(jax.random.fold_in(streams_of[19], 3), TOKENS_B // TOK_B_DEV)
    specialist_picks = jax.vmap(lambda own, number: assign_block(jax.random.fold_in(streams_of[19], 2), own, number, TOK_B_DEV, EXPERTS, TOPK, CAP, 2))(specialist_picks_keys, specialist_picks_turns).reshape((TOKENS_B, TOPK))
    selected_specialist_coefs = jnp.clip(0.1 + 0.9 * jax.random.uniform(streams_of[20], (TOKENS_B, TOPK), jnp.float32) ** shard_levels(streams_of[20], (TOKENS_B, TOPK), ((0, 8),), -0.2, 0.2), 0.1, 1.0)
    return {"blender_incoming_features": blender_incoming_features, "entry_latent_matrix": entry_latent_matrix, "exit_latent_matrix": exit_latent_matrix, "unactivated_valve": unactivated_valve, "presoftplus_strides": presoftplus_strides, "extra_attenuation": extra_attenuation, "incoming_feature_kernel": incoming_feature_kernel, "entry_latent_kernel": entry_latent_kernel, "exit_latent_kernel": exit_latent_kernel, "stride_offset_vector": stride_offset_vector, "attenuation_speed_exponent": attenuation_speed_exponent, "bypass_coef_vector": bypass_coef_vector, "cluster_rescale_coefs": cluster_rescale_coefs, "blender_result_matrix": blender_result_matrix, "latter_microbatch_activations": latter_microbatch_activations, "specialist_rescale_coefs": specialist_rescale_coefs, "specialist_valve_matrix": specialist_valve_matrix, "specialist_expand_matrix": specialist_expand_matrix, "specialist_contract_matrix": specialist_contract_matrix, "specialist_picks": specialist_picks, "selected_specialist_coefs": selected_specialist_coefs}


NORM_EPS = 1e-06
HIGHEST = lax.Precision.HIGHEST

def conv_silu(inputs, weight):
    tap_count = weight.shape[0]
    context_span = inputs.shape[0]
    padded = jnp.pad(inputs.astype(jnp.float32), ((tap_count - 1, 0), (0, 0)))
    kernel = weight.astype(jnp.float32)
    running_total = kernel[0] * padded[0:context_span]
    for offset in range(1, tap_count):
        running_total = running_total + kernel[offset] * padded[offset:offset + context_span]
    return jax.nn.silu(running_total)

def block_step(carry_state, inputs):
    scaled_x, b_block, c_block, log_block = inputs
    context_span = log_block.shape[0]
    running = jnp.cumsum(log_block, axis=0)
    causal = (jnp.arange(context_span)[:, None] >= jnp.arange(context_span)[None, :])[:, :, None, None]
    log_gap = running[:, None] - running[None, :]
    weights = jnp.where(causal, jnp.exp(jnp.where(causal, log_gap, 0.0)), 0.0)
    scores = jnp.einsum('lgn,sgn->lsg', c_block, b_block, preferred_element_type=jnp.float32)
    inside = jnp.einsum('lsgj,sgjp->lgjp', scores[..., None] * weights, scaled_x, precision=HIGHEST)
    c_wide = c_block.astype(jnp.float32)
    b_wide = b_block.astype(jnp.float32)
    before = jnp.einsum('lgn,gjpn->lgjp', c_wide, carry_state, precision=HIGHEST) * jnp.exp(running)[..., None]
    to_end = jnp.exp(running[-1] - running)
    carry_state = carry_state * jnp.exp(running[-1])[..., None, None] + jnp.einsum('sgn,sgjp->gjpn', b_wide, scaled_x * to_end[..., None], precision=HIGHEST)
    return (carry_state, inside + before)

def rounded_pieces(left, right, pieces):
    block_width = left.shape[1] // pieces
    running_total = jnp.zeros((left.shape[0], right.shape[1]), jnp.float32)
    for piece_index in range(pieces):
        block_term = jnp.dot(left[:, piece_index * block_width:(piece_index + 1) * block_width], right[piece_index * block_width:(piece_index + 1) * block_width], preferred_element_type=jnp.float32).astype(jnp.bfloat16)
        running_total = running_total + lax.optimization_barrier(block_term).astype(jnp.float32)
    return running_total.astype(jnp.bfloat16)

def reference(blender_incoming_features, entry_latent_matrix, exit_latent_matrix, unactivated_valve, presoftplus_strides, extra_attenuation, incoming_feature_kernel, entry_latent_kernel, exit_latent_kernel, stride_offset_vector, attenuation_speed_exponent, bypass_coef_vector, cluster_rescale_coefs, blender_result_matrix, latter_microbatch_activations, specialist_rescale_coefs, specialist_valve_matrix, specialist_expand_matrix, specialist_contract_matrix, specialist_picks, selected_specialist_coefs):
    context_span = blender_incoming_features.shape[0]
    members_within_cluster = HEADS // SHARING_CLUSTERS
    conv_x_out = conv_silu(blender_incoming_features, incoming_feature_kernel).reshape(context_span, SHARING_CLUSTERS, members_within_cluster, HEAD_DIM)
    conv_b_out = conv_silu(entry_latent_matrix, entry_latent_kernel).astype(jnp.bfloat16).reshape(context_span, SHARING_CLUSTERS, STATE)
    conv_c_out = conv_silu(exit_latent_matrix, exit_latent_kernel).astype(jnp.bfloat16).reshape(context_span, SHARING_CLUSTERS, STATE)
    stride_amount = jax.nn.softplus(presoftplus_strides + stride_offset_vector[None, :])
    attenuation_exponent = (-jnp.exp(attenuation_speed_exponent)[None, :] * stride_amount + extra_attenuation).reshape(context_span, SHARING_CLUSTERS, members_within_cluster)
    scaled_x = conv_x_out * stride_amount.reshape(context_span, SHARING_CLUSTERS, members_within_cluster)[..., None]
    blocks = context_span // BLOCK

    def as_blocks(array_value):
        return array_value.reshape((blocks, BLOCK) + array_value.shape[1:])
    start_state = jnp.zeros((SHARING_CLUSTERS, members_within_cluster, HEAD_DIM, STATE), jnp.float32)
    _, block_out = lax.scan(block_step, start_state, (as_blocks(scaled_x), as_blocks(conv_b_out), as_blocks(conv_c_out), as_blocks(attenuation_exponent)))
    ssd_out = block_out.reshape(context_span, SHARING_CLUSTERS, members_within_cluster, HEAD_DIM) + bypass_coef_vector.reshape(SHARING_CLUSTERS, members_within_cluster)[None, :, :, None] * conv_x_out
    gated_out = ssd_out.reshape(context_span, INNER) * jax.nn.silu(unactivated_valve.astype(jnp.float32))
    grouped = gated_out.reshape(context_span, SHARING_CLUSTERS, INNER // SHARING_CLUSTERS)
    grouped = grouped * lax.rsqrt(lax.optimization_barrier(jnp.mean(grouped * grouped, axis=-1, keepdims=True)) + NORM_EPS)
    normed = (grouped.reshape(context_span, INNER) * cluster_rescale_coefs.astype(jnp.float32)).astype(jnp.bfloat16)
    mixed_a = rounded_pieces(normed, blender_result_matrix, N_TP)
    widened = latter_microbatch_activations.astype(jnp.float32)
    normed_b = (widened * lax.rsqrt(lax.optimization_barrier(jnp.mean(widened * widened, axis=-1, keepdims=True)) + NORM_EPS) * specialist_rescale_coefs.astype(jnp.float32)).astype(jnp.bfloat16)
    flat_routes = specialist_picks.reshape(-1).astype(jnp.int32)
    assigned = flat_routes.shape[0]
    sorted_order = jnp.argsort(flat_routes, stable=True).astype(jnp.int32)
    routes_sorted = flat_routes[sorted_order]
    tokens_sorted = (sorted_order // TOPK).astype(jnp.int32)
    counts = lax.optimization_barrier(jnp.sum((flat_routes[:, None] == jnp.arange(EXPERTS, dtype=jnp.int32)[None, :]).astype(jnp.int32), axis=0)).astype(jnp.int32)
    starts = (jnp.cumsum(counts) - counts).astype(jnp.int32)
    place_sorted = (jnp.arange(assigned, dtype=jnp.int32) - starts[routes_sorted]).astype(jnp.int32)
    places = jnp.zeros((assigned,), jnp.int32).at[sorted_order].set(place_sorted)
    capacity_all = N_EP * CAP

    def one_expert(expert):
        slots = jnp.arange(capacity_all, dtype=jnp.int32)
        is_valid = slots < counts[expert]
        token_ids = tokens_sorted[jnp.minimum(starts[expert] + slots, assigned - 1)]
        chosen = jnp.where(is_valid[:, None], normed_b[token_ids], jnp.zeros((), jnp.bfloat16))
        gate_sum = jnp.dot(chosen, specialist_valve_matrix[expert], preferred_element_type=jnp.float32)
        up_sum = jnp.dot(chosen, specialist_expand_matrix[expert], preferred_element_type=jnp.float32)
        hidden = (jax.nn.silu(gate_sum) * up_sum).astype(jnp.bfloat16)
        return rounded_pieces(hidden, specialist_contract_matrix[expert], N_TP)
    results = lax.map(one_expert, jnp.arange(EXPERTS, dtype=jnp.int32))
    picked = results[flat_routes, places].astype(jnp.float32) * selected_specialist_coefs.reshape(assigned, 1)
    mixed_b = lax.optimization_barrier(jnp.sum(picked.reshape(assigned // TOPK, TOPK, D), axis=1)).astype(jnp.bfloat16)
    return (mixed_a, mixed_b)
```

```python
import functools

import jax
import jax.numpy as jnp
from jax import lax
from jax.experimental import pallas as pl
from jax.experimental.pallas import tpu as pltpu
from jax.sharding import PartitionSpec as P

HEADS = 64
HEAD_DIM = 64
SHARING_CLUSTERS = 16
STATE = 128
BLOCK = 64
TOPK = 2


NORM_EPS = 1e-06
HIGHEST = lax.Precision.HIGHEST


def from_behind(block, axis, distance):
    devices = range(lax.axis_size(axis))
    route = [(i - distance, i) for i in devices if i - distance in devices]
    return lax.ppermute(block, axis, route)


VMEM = pl.BlockSpec(memory_space=pltpu.VMEM)
HALO = 8
LANES = 128


def silu(v):
    return v / (1.0 + jnp.exp(-v))


def widen(per_head, first, count, rows):
    lane = lax.broadcasted_iota(jnp.int32, (rows, LANES), 1)
    pieces = []
    for h in range(first, first + count, 2):
        left = jnp.broadcast_to(per_head[:, h : h + 1], (rows, LANES))
        right = jnp.broadcast_to(per_head[:, h + 1 : h + 2], (rows, LANES))
        pieces.append(jnp.where(lane < HEAD_DIM, left, right))
    return jnp.concatenate(pieces, axis=1)


def ssd_kernel(
    members,
    x_ref,
    b_ref,
    c_ref,
    rim_ref,
    pre_ref,
    extra_ref,
    kx_ref,
    kb_ref,
    kc_ref,
    offset_ref,
    speed_ref,
    bypass_ref,
    y_ref,
    cc_ref,
    run_ref,
    pieces_ref,
    joined,
    state,
):
    rows, channels = x_ref.shape
    latent = b_ref.shape[1]
    groups = latent // STATE
    wide = members * HEAD_DIM
    taps = kx_ref.shape[0]
    ep_count, piece = pieces_ref.shape[0], pieces_ref.shape[1] - 2

    def conv(ref, k_ref, start, width, rim_start):
        joined[0:HALO, 0:width] = rim_ref[:, rim_start : rim_start + width].astype(jnp.float32)
        joined[HALO : HALO + rows, 0:width] = ref[:, start : start + width].astype(jnp.float32)
        kernel = k_ref[:, start : start + width].astype(jnp.float32)
        total = None
        for j in range(taps):
            at = HALO - taps + 1 + j
            term = kernel[j : j + 1] * joined[at : at + rows, 0:width]
            total = term if total is None else total + term
        return silu(total)

    z = pre_ref[...] + offset_ref[...]
    step = jnp.maximum(z, 0.0) + jnp.log1p(jnp.exp(-jnp.abs(z)))
    decay = -jnp.exp(speed_ref[...]) * step + extra_ref[...]
    row = lax.broadcasted_iota(jnp.int32, (rows, rows), 0)
    col = lax.broadcasted_iota(jnp.int32, (rows, rows), 1)
    causal = row >= col
    tri = causal.astype(jnp.float32)
    run = jnp.dot(tri, decay, preferred_element_type=jnp.float32, precision=HIGHEST)
    run_t = lax.dot_general(
        decay,
        tri,
        (((0,), (1,)), ((), ())),
        preferred_element_type=jnp.float32,
        precision=HIGHEST,
    )
    run_ref[...] = run
    last = run[rows - 1 : rows]
    to_end = jnp.exp(last - run)
    bypass = bypass_ref[...]
    lane = lax.broadcasted_iota(jnp.int32, (rows, LANES), 1)
    for g in range(groups):
        first = g * members
        cols = slice(g * wide, (g + 1) * wide)
        xc = conv(x_ref, kx_ref, g * wide, wide, g * wide)
        bb = conv(b_ref, kb_ref, g * STATE, STATE, channels + g * STATE).astype(jnp.bfloat16)
        cc = conv(c_ref, kc_ref, g * STATE, STATE, channels + latent + g * STATE).astype(jnp.bfloat16)
        cc_ref[:, g * STATE : (g + 1) * STATE] = cc
        xs = xc * widen(step, first, members, rows)
        xs16 = xs.astype(jnp.bfloat16)
        scores = lax.dot_general(
            cc, bb, (((1,), (1,)), ((), ())), preferred_element_type=jnp.float32
        )
        scores = jnp.where(causal, scores, 0.0)
        inside = []
        for pair in range(0, members, 2):
            x_pair = xs16[:, pair * HEAD_DIM : (pair + 2) * HEAD_DIM]
            both = []
            for h in (first + pair, first + pair + 1):
                gap = jnp.minimum(run[:, h : h + 1] - run_t[h : h + 1, :], 0.0)
                weights = (jnp.exp(gap) * scores).astype(jnp.bfloat16)
                both.append(jnp.dot(weights, x_pair, preferred_element_type=jnp.float32))
            inside.append(jnp.where(lane < HEAD_DIM, both[0], both[1]))
        y_ref[:, cols] = jnp.concatenate(inside, axis=1) + xc * widen(bypass, first, members, 1)
        x_end = (xs * widen(to_end, first, members, rows)).astype(jnp.bfloat16)
        state[:, cols] = lax.dot_general(
            bb, x_end, (((0,), (0,)), ((), ())), preferred_element_type=jnp.float32
        )
    for e in range(ep_count):
        pieces_ref[e, 0:piece, :] = state[e * piece : (e + 1) * piece, :].astype(jnp.bfloat16)
    logs = widen(last, 0, groups * members, 1)
    high = logs.astype(jnp.bfloat16)
    low = (logs - high.astype(jnp.float32)).astype(jnp.bfloat16)
    for e in range(ep_count):
        pieces_ref[e, piece : piece + 1, :] = high
        pieces_ref[e, piece + 1 : piece + 2, :] = low


def prefix_kernel(in_ref, out_ref):
    ep_count, piece = in_ref.shape[0], in_ref.shape[1] - 2
    entering = jnp.zeros((piece, in_ref.shape[2]), jnp.float32)
    for d in range(ep_count):
        out_ref[d, :, :] = entering.astype(jnp.bfloat16)
        block = in_ref[d, :, :].astype(jnp.float32)
        log = block[piece : piece + 1] + block[piece + 1 : piece + 2]
        entering = entering * jnp.exp(log) + block[0:piece]


def finish_kernel(
    members, y_ref, cc_ref, run_ref, enter_ref, valve_ref, gain_ref, w_ref, out_ref, normed
):
    rows, channels = y_ref.shape
    wide = members * HEAD_DIM

    @pl.when(pl.program_id(0) == 0)
    def _():
        grown = jnp.exp(run_ref[...])
        for g in range(channels // wide):
            cols = slice(g * wide, (g + 1) * wide)
            carried = jnp.dot(
                cc_ref[:, g * STATE : (g + 1) * STATE],
                enter_ref[:, cols],
                preferred_element_type=jnp.float32,
            )
            ssd = y_ref[:, cols] + carried * widen(grown, g * members, members, rows)
            gated = ssd * silu(valve_ref[:, cols].astype(jnp.float32))
            scale = lax.rsqrt(jnp.mean(gated * gated, axis=1, keepdims=True) + NORM_EPS)
            normed[:, cols] = (gated * scale * gain_ref[:, cols].astype(jnp.float32)).astype(
                jnp.bfloat16
            )

    out_ref[...] = jnp.dot(
        normed[...], w_ref[...], preferred_element_type=jnp.float32
    ).astype(jnp.bfloat16)


def experts_kernel(x_ref, gate_ref, up_ref, down_ref, out_ref, total):
    step = pl.program_id(1)
    rows = x_ref[...]
    gate = jnp.dot(rows, gate_ref[...], preferred_element_type=jnp.float32)
    up = jnp.dot(rows, up_ref[...], preferred_element_type=jnp.float32)
    hidden = (silu(gate) * up).astype(jnp.bfloat16)
    term = jnp.dot(hidden, down_ref[...], preferred_element_type=jnp.float32)
    final = pl.num_programs(1) - 1

    @pl.when(step == 0)
    def _():
        total[...] = term

    @pl.when(step > 0)
    def _():
        total[...] += term

    @pl.when(step == final)
    def _():
        out_ref[...] = total[...].astype(jnp.bfloat16)


def run_experts(rows, gate, up, down):
    experts, count, width = rows.shape
    units = gate.shape[2]
    tile = min(256, units)
    return pl.pallas_call(
        experts_kernel,
        grid=(experts, units // tile),
        in_specs=[
            pl.BlockSpec((None, count, width), lambda e, f: (e, 0, 0)),
            pl.BlockSpec((None, width, tile), lambda e, f: (e, 0, f)),
            pl.BlockSpec((None, width, tile), lambda e, f: (e, 0, f)),
            pl.BlockSpec((None, tile, width), lambda e, f: (e, f, 0)),
        ],
        out_specs=pl.BlockSpec((None, count, width), lambda e, f: (e, 0, 0)),
        out_shape=jax.ShapeDtypeStruct((experts, count, width), jnp.bfloat16),
        scratch_shapes=[pltpu.VMEM((count, width), jnp.float32)],
        cost_estimate=pl.CostEstimate(
            flops=6 * experts * count * width * units,
            bytes_accessed=2 * experts * (2 * count * width + 3 * width * units),
            transcendentals=experts * count * units,
        ),
        compiler_params=pltpu.CompilerParams(
            dimension_semantics=("arbitrary", "arbitrary"), vmem_limit_bytes=48 * 1024 * 1024
        ),
        name="experts",
    )(rows, gate, up, down)


def local(
    blender_incoming_features,
    entry_latent_matrix,
    exit_latent_matrix,
    unactivated_valve,
    presoftplus_strides,
    extra_attenuation,
    incoming_feature_kernel,
    entry_latent_kernel,
    exit_latent_kernel,
    stride_offset_vector,
    attenuation_speed_exponent,
    bypass_coef_vector,
    cluster_rescale_coefs,
    blender_result_matrix,
    latter_microbatch_activations,
    specialist_rescale_coefs,
    specialist_valve_matrix,
    specialist_expand_matrix,
    specialist_contract_matrix,
    specialist_picks,
    selected_specialist_coefs,
):
    tap_count = incoming_feature_kernel.shape[0]
    tok_rows = blender_incoming_features.shape[0]
    members_within_cluster = HEADS // SHARING_CLUSTERS
    ep_count = lax.axis_size("ep")
    channels = blender_incoming_features.shape[1]
    latent = entry_latent_matrix.shape[1]
    heads_local = presoftplus_strides.shape[1]
    piece = STATE // ep_count
    tail = tok_rows - HALO
    rim = from_behind(
        jnp.concatenate(
            [
                blender_incoming_features[tail:],
                entry_latent_matrix[tail:],
                exit_latent_matrix[tail:],
            ],
            axis=1,
        ),
        "ep",
        1,
    )
    block_out, conv_c_out, running, pieces = pl.pallas_call(
        functools.partial(ssd_kernel, members_within_cluster),
        in_specs=[VMEM] * 12,
        out_specs=[VMEM] * 4,
        out_shape=[
            jax.ShapeDtypeStruct((tok_rows, channels), jnp.float32),
            jax.ShapeDtypeStruct((tok_rows, latent), jnp.bfloat16),
            jax.ShapeDtypeStruct((tok_rows, heads_local), jnp.float32),
            jax.ShapeDtypeStruct((ep_count, piece + 2, channels), jnp.bfloat16),
        ],
        scratch_shapes=[
            pltpu.VMEM((tok_rows + HALO, members_within_cluster * HEAD_DIM), jnp.float32),
            pltpu.VMEM((STATE, channels), jnp.float32),
        ],
        cost_estimate=pl.CostEstimate(
            flops=2 * tok_rows * tok_rows * channels * 8,
            bytes_accessed=6 * tok_rows * channels * 2,
            transcendentals=tok_rows * tok_rows * heads_local,
        ),
        name="ssd_local",
    )(
        blender_incoming_features,
        entry_latent_matrix,
        exit_latent_matrix,
        rim,
        presoftplus_strides,
        extra_attenuation,
        incoming_feature_kernel,
        entry_latent_kernel,
        exit_latent_kernel,
        stride_offset_vector[None, :],
        attenuation_speed_exponent[None, :],
        bypass_coef_vector[None, :],
    )
    spread = lax.all_to_all(pieces, "ep", split_axis=0, concat_axis=0, tiled=True)
    entering = pl.pallas_call(
        prefix_kernel,
        in_specs=[VMEM],
        out_specs=VMEM,
        out_shape=jax.ShapeDtypeStruct((ep_count, piece, channels), jnp.bfloat16),
        name="state_prefix",
    )(spread)
    enter_state = lax.all_to_all(entering, "ep", split_axis=0, concat_axis=0, tiled=True).reshape(
        STATE, channels
    )
    width_a = blender_result_matrix.shape[1]
    tile_a = min(512, width_a)
    whole = lambda *shape: pl.BlockSpec(shape, lambda i: (0,) * len(shape))
    partial_a = pl.pallas_call(
        functools.partial(finish_kernel, members_within_cluster),
        grid=(width_a // tile_a,),
        in_specs=[
            whole(tok_rows, channels),
            whole(tok_rows, latent),
            whole(tok_rows, heads_local),
            whole(STATE, channels),
            whole(tok_rows, channels),
            whole(1, channels),
            pl.BlockSpec((channels, tile_a), lambda i: (0, i)),
        ],
        out_specs=pl.BlockSpec((tok_rows, tile_a), lambda i: (0, i)),
        out_shape=jax.ShapeDtypeStruct((tok_rows, width_a), jnp.bfloat16),
        scratch_shapes=[pltpu.VMEM((tok_rows, channels), jnp.bfloat16)],
        cost_estimate=pl.CostEstimate(
            flops=2 * tok_rows * channels * (width_a + 4 * STATE),
            bytes_accessed=2 * channels * (width_a + 4 * tok_rows) + 2 * tok_rows * width_a,
            transcendentals=2 * tok_rows * channels,
        ),
        compiler_params=pltpu.CompilerParams(dimension_semantics=("arbitrary",)),
        name="finish_mixer",
    )(
        block_out,
        conv_c_out,
        running,
        enter_state,
        unactivated_valve,
        cluster_rescale_coefs[None, :],
        blender_result_matrix,
    )
    mixed_a = lax.psum_scatter(partial_a, "tp", scatter_dimension=0, tiled=True)
    token_count = latter_microbatch_activations.shape[0]
    model_width = latter_microbatch_activations.shape[1]
    local_experts = specialist_valve_matrix.shape[0]
    expert_count = ep_count * local_experts
    capacity = 3 * token_count * TOPK // (2 * expert_count)
    slot_total = expert_count * capacity
    widened = latter_microbatch_activations.astype(jnp.float32)
    normed_b = (
        widened
        * lax.rsqrt(jnp.mean(widened * widened, axis=-1, keepdims=True) + NORM_EPS)
        * specialist_rescale_coefs.astype(jnp.float32)
    ).astype(jnp.bfloat16)
    flat_routes = specialist_picks.reshape(-1)
    assigned = flat_routes.shape[0]
    positions = jnp.arange(assigned, dtype=jnp.int32)
    earlier_same = (flat_routes[:, None] == flat_routes[None, :]) & (
        positions[None, :] < positions[:, None]
    )
    slot_rank = jnp.sum(earlier_same.astype(jnp.int32), axis=1)
    slot_of = flat_routes * capacity + slot_rank
    slot_ids = jnp.arange(slot_total, dtype=jnp.int32)
    placing = (slot_ids[:, None] == slot_of[None, :]).astype(jnp.bfloat16)
    placing = jnp.sum(placing.reshape(slot_total, token_count, TOPK), axis=2)
    outgoing = jnp.dot(placing, normed_b, preferred_element_type=jnp.float32).astype(jnp.bfloat16)
    outgoing = outgoing.reshape(ep_count, local_experts, capacity, model_width)
    arrived = lax.all_to_all(outgoing, "ep", split_axis=0, concat_axis=0, tiled=True)
    arrived_rows = arrived.transpose(1, 0, 2, 3).reshape(
        local_experts, ep_count * capacity, model_width
    )
    partial_out = run_experts(
        arrived_rows,
        specialist_valve_matrix,
        specialist_expand_matrix,
        specialist_contract_matrix,
    )
    partial_out = partial_out.reshape(local_experts, ep_count, capacity, model_width)
    partial_out = partial_out.transpose(1, 0, 2, 3)
    summed = lax.psum_scatter(
        partial_out, "tp", scatter_dimension=3, tiled=True
    )
    returned = lax.all_to_all(summed, "ep", split_axis=0, concat_axis=0, tiled=True)
    returned = returned.reshape(slot_total, -1)
    token_slots = slot_of.reshape(token_count, TOPK)
    combined = jnp.zeros((token_count, returned.shape[1]), jnp.float32)
    for pick_index in range(TOPK):
        selecting = (token_slots[:, pick_index][:, None] == slot_ids[None, :]).astype(jnp.bfloat16)
        chosen_rows = jnp.dot(selecting, returned, preferred_element_type=jnp.float32)
        combined = combined + chosen_rows * selected_specialist_coefs[:, pick_index][:, None]
    mixed_b = combined.astype(jnp.bfloat16)
    return (mixed_a, mixed_b)


def solution(mesh):
    in_specs = (
        P("ep", "tp"),
        P("ep", "tp"),
        P("ep", "tp"),
        P("ep", "tp"),
        P("ep", "tp"),
        P("ep", "tp"),
        P(None, "tp"),
        P(None, "tp"),
        P(None, "tp"),
        P("tp"),
        P("tp"),
        P("tp"),
        P("tp"),
        P("tp", None),
        P("ep", None),
        P(),
        P("ep", None, "tp"),
        P("ep", None, "tp"),
        P("ep", "tp", None),
        P("ep", None),
        P("ep", None),
    )
    out_specs = (P(("ep", "tp"), None), P("ep", "tp"))
    return jax.shard_map(local, mesh=mesh, in_specs=in_specs, out_specs=out_specs, check_vma=False)
```

```python
import functools

import jax
import jax.numpy as jnp
from jax import lax
from jax.experimental import pallas as pl
from jax.experimental.pallas import tpu as pltpu
from jax.sharding import PartitionSpec as P

HEADS = 64
HEAD_DIM = 64
SHARING_CLUSTERS = 16
STATE = 128
BLOCK = 64
TOPK = 2


NORM_EPS = 1e-06
HIGHEST = lax.Precision.HIGHEST


def from_behind(block, axis, distance):
    devices = range(lax.axis_size(axis))
    route = [(i - distance, i) for i in devices if i - distance in devices]
    return lax.ppermute(block, axis, route)


VMEM = pl.BlockSpec(memory_space=pltpu.VMEM)
HALO = 8
LANES = 128


def silu(v):
    return v / (1.0 + jnp.exp(-v))


def widen(per_head, first, count, rows):
    lane = lax.broadcasted_iota(jnp.int32, (rows, LANES), 1)
    pieces = []
    for h in range(first, first + count, 2):
        left = jnp.broadcast_to(per_head[:, h : h + 1], (rows, LANES))
        right = jnp.broadcast_to(per_head[:, h + 1 : h + 2], (rows, LANES))
        pieces.append(jnp.where(lane < HEAD_DIM, left, right))
    return jnp.concatenate(pieces, axis=1)


def ssd_kernel(
    members,
    x_ref,
    b_ref,
    c_ref,
    rim_ref,
    pre_ref,
    extra_ref,
    kx_ref,
    kb_ref,
    kc_ref,
    offset_ref,
    speed_ref,
    bypass_ref,
    y_ref,
    cc_ref,
    run_ref,
    pieces_ref,
    joined,
    state,
):
    rows, channels = x_ref.shape
    latent = b_ref.shape[1]
    groups = latent // STATE
    wide = members * HEAD_DIM
    taps = kx_ref.shape[0]
    ep_count, piece = pieces_ref.shape[0], pieces_ref.shape[1] - 2

    def conv(ref, k_ref, start, width, rim_start):
        joined[0:HALO, 0:width] = rim_ref[:, rim_start : rim_start + width].astype(jnp.float32)
        joined[HALO : HALO + rows, 0:width] = ref[:, start : start + width].astype(jnp.float32)
        kernel = k_ref[:, start : start + width].astype(jnp.float32)
        total = None
        for j in range(taps):
            at = HALO - taps + 1 + j
            term = kernel[j : j + 1] * joined[at : at + rows, 0:width]
            total = term if total is None else total + term
        return silu(total)

    z = pre_ref[...] + offset_ref[...]
    step = jnp.maximum(z, 0.0) + jnp.log1p(jnp.exp(-jnp.abs(z)))
    decay = -jnp.exp(speed_ref[...]) * step + extra_ref[...]
    row = lax.broadcasted_iota(jnp.int32, (rows, rows), 0)
    col = lax.broadcasted_iota(jnp.int32, (rows, rows), 1)
    causal = row >= col
    tri = causal.astype(jnp.float32)
    run = jnp.dot(tri, decay, preferred_element_type=jnp.float32, precision=HIGHEST)
    run_t = lax.dot_general(
        decay,
        tri,
        (((0,), (1,)), ((), ())),
        preferred_element_type=jnp.float32,
        precision=HIGHEST,
    )
    run_ref[...] = run
    last = run[rows - 1 : rows]
    to_end = jnp.exp(last - run)
    bypass = bypass_ref[...]
    lane = lax.broadcasted_iota(jnp.int32, (rows, LANES), 1)
    for g in range(groups):
        first = g * members
        cols = slice(g * wide, (g + 1) * wide)
        xc = conv(x_ref, kx_ref, g * wide, wide, g * wide)
        bb = conv(b_ref, kb_ref, g * STATE, STATE, channels + g * STATE).astype(jnp.bfloat16)
        cc = conv(c_ref, kc_ref, g * STATE, STATE, channels + latent + g * STATE).astype(jnp.bfloat16)
        cc_ref[:, g * STATE : (g + 1) * STATE] = cc
        xs = xc * widen(step, first, members, rows)
        xs16 = xs.astype(jnp.bfloat16)
        scores = lax.dot_general(
            cc, bb, (((1,), (1,)), ((), ())), preferred_element_type=jnp.float32
        )
        scores = jnp.where(causal, scores, 0.0)
        inside = []
        for pair in range(0, members, 2):
            x_pair = xs16[:, pair * HEAD_DIM : (pair + 2) * HEAD_DIM]
            both = []
            for h in (first + pair, first + pair + 1):
                gap = jnp.minimum(run[:, h : h + 1] - run_t[h : h + 1, :], 0.0)
                weights = (jnp.exp(gap) * scores).astype(jnp.bfloat16)
                both.append(jnp.dot(weights, x_pair, preferred_element_type=jnp.float32))
            inside.append(jnp.where(lane < HEAD_DIM, both[0], both[1]))
        y_ref[:, cols] = jnp.concatenate(inside, axis=1) + xc * widen(bypass, first, members, 1)
        x_end = (xs * widen(to_end, first, members, rows)).astype(jnp.bfloat16)
        state[:, cols] = lax.dot_general(
            bb, x_end, (((0,), (0,)), ((), ())), preferred_element_type=jnp.float32
        )
    for e in range(ep_count):
        pieces_ref[e, 0:piece, :] = state[e * piece : (e + 1) * piece, :].astype(jnp.bfloat16)
    logs = widen(last, 0, groups * members, 1)
    high = logs.astype(jnp.bfloat16)
    low = (logs - high.astype(jnp.float32)).astype(jnp.bfloat16)
    for e in range(ep_count):
        pieces_ref[e, piece : piece + 1, :] = high
        pieces_ref[e, piece + 1 : piece + 2, :] = low


def prefix_kernel(in_ref, out_ref):
    ep_count, piece = in_ref.shape[0], in_ref.shape[1] - 2
    entering = jnp.zeros((piece, in_ref.shape[2]), jnp.float32)
    for d in range(ep_count):
        out_ref[d, :, :] = entering.astype(jnp.bfloat16)
        block = in_ref[d, :, :].astype(jnp.float32)
        log = block[piece : piece + 1] + block[piece + 1 : piece + 2]
        entering = entering * jnp.exp(log) + block[0:piece]


def finish_kernel(
    members, y_ref, cc_ref, run_ref, enter_ref, valve_ref, gain_ref, w_ref, out_ref, normed
):
    rows, channels = y_ref.shape
    wide = members * HEAD_DIM

    @pl.when(pl.program_id(0) == 0)
    def _():
        grown = jnp.exp(run_ref[...])
        for g in range(channels // wide):
            cols = slice(g * wide, (g + 1) * wide)
            carried = jnp.dot(
                cc_ref[:, g * STATE : (g + 1) * STATE],
                enter_ref[:, cols],
                preferred_element_type=jnp.float32,
            )
            ssd = y_ref[:, cols] + carried * widen(grown, g * members, members, rows)
            gated = ssd * silu(valve_ref[:, cols].astype(jnp.float32))
            scale = lax.rsqrt(jnp.mean(gated * gated, axis=1, keepdims=True) + NORM_EPS)
            normed[:, cols] = (gated * scale * gain_ref[:, cols].astype(jnp.float32)).astype(
                jnp.bfloat16
            )

    out_ref[...] = jnp.dot(
        normed[...], w_ref[...], preferred_element_type=jnp.float32
    ).astype(jnp.bfloat16)


def experts_kernel(x_ref, gate_ref, up_ref, down_ref, out_ref, total):
    step = pl.program_id(1)
    parts, _, depth = x_ref.shape
    gate = up = 0.0
    for p in range(parts):
        rows = x_ref[p]
        deep = slice(p * depth, (p + 1) * depth)
        gate += jnp.dot(rows, gate_ref[deep, :], preferred_element_type=jnp.float32)
        up += jnp.dot(rows, up_ref[deep, :], preferred_element_type=jnp.float32)
    hidden = (silu(gate) * up).astype(jnp.bfloat16)
    term = jnp.dot(hidden, down_ref[...], preferred_element_type=jnp.float32)
    final = pl.num_programs(1) - 1

    @pl.when(step == 0)
    def _():
        total[...] = term

    @pl.when(step > 0)
    def _():
        total[...] += term

    @pl.when(step == final)
    def _():
        for p in range(parts):
            out_ref[p] = total[:, p * depth : (p + 1) * depth].astype(jnp.bfloat16)


def run_experts(rows, gate, up, down):
    parts, experts, count, depth = rows.shape
    width = parts * depth
    units = gate.shape[2]
    tile = min(256, units)
    return pl.pallas_call(
        experts_kernel,
        grid=(experts, units // tile),
        in_specs=[
            pl.BlockSpec((parts, None, count, depth), lambda e, f: (0, e, 0, 0)),
            pl.BlockSpec((None, width, tile), lambda e, f: (e, 0, f)),
            pl.BlockSpec((None, width, tile), lambda e, f: (e, 0, f)),
            pl.BlockSpec((None, tile, width), lambda e, f: (e, f, 0)),
        ],
        out_specs=pl.BlockSpec((parts, None, count, depth), lambda e, f: (0, e, 0, 0)),
        out_shape=jax.ShapeDtypeStruct((parts, experts, count, depth), jnp.bfloat16),
        scratch_shapes=[pltpu.VMEM((count, width), jnp.float32)],
        cost_estimate=pl.CostEstimate(
            flops=6 * experts * count * width * units,
            bytes_accessed=2 * experts * (2 * count * width + 3 * width * units),
            transcendentals=experts * count * units,
        ),
        compiler_params=pltpu.CompilerParams(
            dimension_semantics=("arbitrary", "arbitrary"), vmem_limit_bytes=48 * 1024 * 1024
        ),
        name="experts",
    )(rows, gate, up, down)


def local(
    blender_incoming_features,
    entry_latent_matrix,
    exit_latent_matrix,
    unactivated_valve,
    presoftplus_strides,
    extra_attenuation,
    incoming_feature_kernel,
    entry_latent_kernel,
    exit_latent_kernel,
    stride_offset_vector,
    attenuation_speed_exponent,
    bypass_coef_vector,
    cluster_rescale_coefs,
    blender_result_matrix,
    latter_microbatch_activations,
    specialist_rescale_coefs,
    specialist_valve_matrix,
    specialist_expand_matrix,
    specialist_contract_matrix,
    specialist_picks,
    selected_specialist_coefs,
):
    tap_count = incoming_feature_kernel.shape[0]
    tok_rows = blender_incoming_features.shape[0]
    members_within_cluster = HEADS // SHARING_CLUSTERS
    ep_count = lax.axis_size("ep")
    channels = blender_incoming_features.shape[1]
    latent = entry_latent_matrix.shape[1]
    heads_local = presoftplus_strides.shape[1]
    piece = STATE // ep_count
    tail = tok_rows - HALO
    rim = from_behind(
        jnp.concatenate(
            [
                blender_incoming_features[tail:],
                entry_latent_matrix[tail:],
                exit_latent_matrix[tail:],
            ],
            axis=1,
        ),
        "ep",
        1,
    )
    block_out, conv_c_out, running, pieces = pl.pallas_call(
        functools.partial(ssd_kernel, members_within_cluster),
        in_specs=[VMEM] * 12,
        out_specs=[VMEM] * 4,
        out_shape=[
            jax.ShapeDtypeStruct((tok_rows, channels), jnp.float32),
            jax.ShapeDtypeStruct((tok_rows, latent), jnp.bfloat16),
            jax.ShapeDtypeStruct((tok_rows, heads_local), jnp.float32),
            jax.ShapeDtypeStruct((ep_count, piece + 2, channels), jnp.bfloat16),
        ],
        scratch_shapes=[
            pltpu.VMEM((tok_rows + HALO, members_within_cluster * HEAD_DIM), jnp.float32),
            pltpu.VMEM((STATE, channels), jnp.float32),
        ],
        cost_estimate=pl.CostEstimate(
            flops=2 * tok_rows * tok_rows * channels * 64,
            bytes_accessed=6 * tok_rows * channels * 2,
            transcendentals=tok_rows * tok_rows * heads_local,
        ),
        name="ssd_local",
    )(
        blender_incoming_features,
        entry_latent_matrix,
        exit_latent_matrix,
        rim,
        presoftplus_strides,
        extra_attenuation,
        incoming_feature_kernel,
        entry_latent_kernel,
        exit_latent_kernel,
        stride_offset_vector[None, :],
        attenuation_speed_exponent[None, :],
        bypass_coef_vector[None, :],
    )
    token_count = latter_microbatch_activations.shape[0]
    model_width = latter_microbatch_activations.shape[1]
    local_experts = specialist_valve_matrix.shape[0]
    expert_count = ep_count * local_experts
    capacity = 3 * token_count * TOPK // (2 * expert_count)
    slot_total = expert_count * capacity
    widened = latter_microbatch_activations.astype(jnp.float32)
    share = model_width // lax.axis_size("tp")
    own = lax.axis_index("tp") * share
    normed_b = (
        lax.dynamic_slice_in_dim(latter_microbatch_activations, own, share, 1).astype(jnp.float32)
        * lax.rsqrt(jnp.mean(widened * widened, axis=-1, keepdims=True) + NORM_EPS)
        * lax.dynamic_slice_in_dim(specialist_rescale_coefs, own, share, 0).astype(jnp.float32)
    ).astype(jnp.bfloat16)
    flat_routes = specialist_picks.reshape(-1)
    assigned = flat_routes.shape[0]
    positions = jnp.arange(assigned, dtype=jnp.int32)
    earlier_same = (flat_routes[:, None] == flat_routes[None, :]) & (
        positions[None, :] < positions[:, None]
    )
    slot_rank = jnp.sum(earlier_same.astype(jnp.int32), axis=1)
    slot_of = flat_routes * capacity + slot_rank
    slot_ids = jnp.arange(slot_total, dtype=jnp.int32)
    placing = (slot_ids[:, None] == slot_of[None, :]).astype(jnp.bfloat16)
    placing = jnp.sum(placing.reshape(slot_total, token_count, TOPK), axis=2)
    outgoing = jnp.dot(placing, normed_b, preferred_element_type=jnp.float32).astype(jnp.bfloat16)
    outgoing = outgoing.reshape(ep_count, local_experts, capacity, share)
    chunks = 2 if capacity % 32 == 0 else 1
    size = capacity // chunks
    gathered = []
    for k in range(chunks):
        arrived = lax.all_to_all(
            outgoing[:, :, k * size : (k + 1) * size],
            "ep",
            split_axis=0,
            concat_axis=0,
            tiled=True,
        )
        arrived_rows = arrived.transpose(1, 0, 2, 3).reshape(local_experts, ep_count * size, share)
        gathered.append(lax.all_gather(arrived_rows, "tp"))
    spread = None
    partials = []
    for k in range(chunks):
        if spread is None:
            gathered[k], pieces = lax.optimization_barrier((gathered[k], pieces))
        else:
            gathered[k], spread = lax.optimization_barrier((gathered[k], spread))
        partial_out = run_experts(
            gathered[k],
            specialist_valve_matrix,
            specialist_expand_matrix,
            specialist_contract_matrix,
        )
        if spread is None:
            partial_out, pieces = lax.optimization_barrier((partial_out, pieces))
            spread = lax.all_to_all(pieces, "ep", split_axis=0, concat_axis=0, tiled=True)
        else:
            partial_out, spread = lax.optimization_barrier((partial_out, spread))
        partials.append(partial_out)
    back = []
    for k in range(chunks):
        summed = lax.psum_scatter(partials[k], "tp", scatter_dimension=0, tiled=False)
        summed = summed.reshape(local_experts, ep_count, size, share).transpose(1, 0, 2, 3)
        back.append(lax.all_to_all(summed, "ep", split_axis=0, concat_axis=0, tiled=True))
    returned = back[0] if chunks == 1 else jnp.concatenate(back, axis=2)
    entering = pl.pallas_call(
        prefix_kernel,
        in_specs=[VMEM],
        out_specs=VMEM,
        out_shape=jax.ShapeDtypeStruct((ep_count, piece, channels), jnp.bfloat16),
        name="state_prefix",
    )(spread)
    enter_state = lax.all_to_all(entering, "ep", split_axis=0, concat_axis=0, tiled=True).reshape(
        STATE, channels
    )
    width_a = blender_result_matrix.shape[1]
    tile_a = min(512, width_a)
    whole = lambda *shape: pl.BlockSpec(shape, lambda i: (0,) * len(shape))
    partial_a = pl.pallas_call(
        functools.partial(finish_kernel, members_within_cluster),
        grid=(width_a // tile_a,),
        in_specs=[
            whole(tok_rows, channels),
            whole(tok_rows, latent),
            whole(tok_rows, heads_local),
            whole(STATE, channels),
            whole(tok_rows, channels),
            whole(1, channels),
            pl.BlockSpec((channels, tile_a), lambda i: (0, i)),
        ],
        out_specs=pl.BlockSpec((tok_rows, tile_a), lambda i: (0, i)),
        out_shape=jax.ShapeDtypeStruct((tok_rows, width_a), jnp.bfloat16),
        scratch_shapes=[pltpu.VMEM((tok_rows, channels), jnp.bfloat16)],
        cost_estimate=pl.CostEstimate(
            flops=8 * tok_rows * channels * (width_a + 4 * STATE),
            bytes_accessed=2 * channels * (width_a + 4 * tok_rows) + 2 * tok_rows * width_a,
            transcendentals=2 * tok_rows * channels,
        ),
        compiler_params=pltpu.CompilerParams(dimension_semantics=("arbitrary",)),
        name="finish_mixer",
    )(
        block_out,
        conv_c_out,
        running,
        enter_state,
        unactivated_valve,
        cluster_rescale_coefs[None, :],
        blender_result_matrix,
    )
    mixed_a = lax.psum_scatter(partial_a, "tp", scatter_dimension=0, tiled=True)
    returned = returned.reshape(slot_total, -1)
    token_slots = slot_of.reshape(token_count, TOPK)
    combined = jnp.zeros((token_count, returned.shape[1]), jnp.float32)
    for pick_index in range(TOPK):
        selecting = (token_slots[:, pick_index][:, None] == slot_ids[None, :]).astype(jnp.bfloat16)
        chosen_rows = jnp.dot(selecting, returned, preferred_element_type=jnp.float32)
        combined = combined + chosen_rows * selected_specialist_coefs[:, pick_index][:, None]
    mixed_b = combined.astype(jnp.bfloat16)
    return (mixed_a, mixed_b)


def solution(mesh):
    in_specs = (
        P("ep", "tp"),
        P("ep", "tp"),
        P("ep", "tp"),
        P("ep", "tp"),
        P("ep", "tp"),
        P("ep", "tp"),
        P(None, "tp"),
        P(None, "tp"),
        P(None, "tp"),
        P("tp"),
        P("tp"),
        P("tp"),
        P("tp"),
        P("tp", None),
        P("ep", None),
        P(),
        P("ep", None, "tp"),
        P("ep", None, "tp"),
        P("ep", "tp", None),
        P("ep", None),
        P("ep", None),
    )
    out_specs = (P(("ep", "tp"), None), P("ep", "tp"))
    return jax.shard_map(local, mesh=mesh, in_specs=in_specs, out_specs=out_specs, check_vma=False)
```

```python
import functools

import jax
import jax.numpy as jnp
from jax import lax
from jax.experimental import pallas as pl
from jax.experimental.pallas import tpu as pltpu
from jax.sharding import PartitionSpec as P

HEADS = 64
HEAD_DIM = 64
SHARING_CLUSTERS = 16
STATE = 128
BLOCK = 64
TOPK = 2


NORM_EPS = 1e-06
HIGHEST = lax.Precision.HIGHEST


def from_behind(block, axis, distance):
    devices = range(lax.axis_size(axis))
    route = [(i - distance, i) for i in devices if i - distance in devices]
    return lax.ppermute(block, axis, route)


VMEM = pl.BlockSpec(memory_space=pltpu.VMEM)
HALO = 8
LANES = 128


def silu(v):
    return v / (1.0 + jnp.exp(-v))


def widen(per_head, first, count, rows):
    lane = lax.broadcasted_iota(jnp.int32, (rows, LANES), 1)
    pieces = []
    for h in range(first, first + count, 2):
        left = jnp.broadcast_to(per_head[:, h : h + 1], (rows, LANES))
        right = jnp.broadcast_to(per_head[:, h + 1 : h + 2], (rows, LANES))
        pieces.append(jnp.where(lane < HEAD_DIM, left, right))
    return jnp.concatenate(pieces, axis=1)


def ssd_kernel(
    members,
    x_ref,
    b_ref,
    c_ref,
    rim_ref,
    pre_ref,
    extra_ref,
    kx_ref,
    kb_ref,
    kc_ref,
    offset_ref,
    speed_ref,
    bypass_ref,
    y_ref,
    cc_ref,
    run_ref,
    pieces_ref,
    joined,
    state,
):
    rows, channels = x_ref.shape
    latent = b_ref.shape[1]
    groups = latent // STATE
    wide = members * HEAD_DIM
    taps = kx_ref.shape[0]
    ep_count, piece = pieces_ref.shape[0], pieces_ref.shape[1] - 2

    def conv(ref, k_ref, start, width, rim_start):
        joined[0:HALO, 0:width] = rim_ref[:, rim_start : rim_start + width].astype(jnp.float32)
        joined[HALO : HALO + rows, 0:width] = ref[:, start : start + width].astype(jnp.float32)
        kernel = k_ref[:, start : start + width].astype(jnp.float32)
        total = None
        for j in range(taps):
            at = HALO - taps + 1 + j
            term = kernel[j : j + 1] * joined[at : at + rows, 0:width]
            total = term if total is None else total + term
        return silu(total)

    z = pre_ref[...] + offset_ref[...]
    step = jnp.maximum(z, 0.0) + jnp.log1p(jnp.exp(-jnp.abs(z)))
    decay = -jnp.exp(speed_ref[...]) * step + extra_ref[...]
    row = lax.broadcasted_iota(jnp.int32, (rows, rows), 0)
    col = lax.broadcasted_iota(jnp.int32, (rows, rows), 1)
    causal = row >= col
    tri = causal.astype(jnp.float32)
    run = jnp.dot(tri, decay, preferred_element_type=jnp.float32, precision=HIGHEST)
    run_t = lax.dot_general(
        decay,
        tri,
        (((0,), (1,)), ((), ())),
        preferred_element_type=jnp.float32,
        precision=HIGHEST,
    )
    run_ref[...] = run
    last = run[rows - 1 : rows]
    to_end = jnp.exp(last - run)
    bypass = bypass_ref[...]
    lane = lax.broadcasted_iota(jnp.int32, (rows, LANES), 1)
    for g in range(groups):
        first = g * members
        cols = slice(g * wide, (g + 1) * wide)
        xc = conv(x_ref, kx_ref, g * wide, wide, g * wide)
        bb = conv(b_ref, kb_ref, g * STATE, STATE, channels + g * STATE).astype(jnp.bfloat16)
        cc = conv(c_ref, kc_ref, g * STATE, STATE, channels + latent + g * STATE).astype(jnp.bfloat16)
        cc_ref[:, g * STATE : (g + 1) * STATE] = cc
        xs = xc * widen(step, first, members, rows)
        xs16 = xs.astype(jnp.bfloat16)
        scores = lax.dot_general(
            cc, bb, (((1,), (1,)), ((), ())), preferred_element_type=jnp.float32
        )
        scores = jnp.where(causal, scores, 0.0)
        inside = []
        for pair in range(0, members, 2):
            x_pair = xs16[:, pair * HEAD_DIM : (pair + 2) * HEAD_DIM]
            both = []
            for h in (first + pair, first + pair + 1):
                gap = jnp.minimum(run[:, h : h + 1] - run_t[h : h + 1, :], 0.0)
                weights = (jnp.exp(gap) * scores).astype(jnp.bfloat16)
                both.append(jnp.dot(weights, x_pair, preferred_element_type=jnp.float32))
            inside.append(jnp.where(lane < HEAD_DIM, both[0], both[1]))
        y_ref[:, cols] = jnp.concatenate(inside, axis=1) + xc * widen(bypass, first, members, 1)
        x_end = (xs * widen(to_end, first, members, rows)).astype(jnp.bfloat16)
        state[:, cols] = lax.dot_general(
            bb, x_end, (((0,), (0,)), ((), ())), preferred_element_type=jnp.float32
        )
    for e in range(ep_count):
        pieces_ref[e, 0:piece, :] = state[e * piece : (e + 1) * piece, :].astype(jnp.bfloat16)
    logs = widen(last, 0, groups * members, 1)
    high = logs.astype(jnp.bfloat16)
    low = (logs - high.astype(jnp.float32)).astype(jnp.bfloat16)
    for e in range(ep_count):
        pieces_ref[e, piece : piece + 1, :] = high
        pieces_ref[e, piece + 1 : piece + 2, :] = low


def prefix_kernel(in_ref, out_ref):
    ep_count, piece = in_ref.shape[0], in_ref.shape[1] - 2
    entering = jnp.zeros((piece, in_ref.shape[2]), jnp.float32)
    for d in range(ep_count):
        out_ref[d, :, :] = entering.astype(jnp.bfloat16)
        block = in_ref[d, :, :].astype(jnp.float32)
        log = block[piece : piece + 1] + block[piece + 1 : piece + 2]
        entering = entering * jnp.exp(log) + block[0:piece]


def finish_kernel(
    members, y_ref, cc_ref, run_ref, enter_ref, valve_ref, gain_ref, w_ref, out_ref, normed
):
    rows, channels = y_ref.shape
    wide = members * HEAD_DIM

    @pl.when(pl.program_id(0) == 0)
    def _():
        grown = jnp.exp(run_ref[...])
        for g in range(channels // wide):
            cols = slice(g * wide, (g + 1) * wide)
            carried = jnp.dot(
                cc_ref[:, g * STATE : (g + 1) * STATE],
                enter_ref[:, cols],
                preferred_element_type=jnp.float32,
            )
            ssd = y_ref[:, cols] + carried * widen(grown, g * members, members, rows)
            gated = ssd * silu(valve_ref[:, cols].astype(jnp.float32))
            scale = lax.rsqrt(jnp.mean(gated * gated, axis=1, keepdims=True) + NORM_EPS)
            normed[:, cols] = (gated * scale * gain_ref[:, cols].astype(jnp.float32)).astype(
                jnp.bfloat16
            )

    out_ref[...] = jnp.dot(
        normed[...], w_ref[...], preferred_element_type=jnp.float32
    ).astype(jnp.bfloat16)


def experts_kernel(x_ref, gate_ref, up_ref, down_ref, out_ref, total):
    step = pl.program_id(1)
    parts, _, depth = x_ref.shape
    gate = up = 0.0
    for p in range(parts):
        rows = x_ref[p]
        deep = slice(p * depth, (p + 1) * depth)
        gate += jnp.dot(rows, gate_ref[deep, :], preferred_element_type=jnp.float32)
        up += jnp.dot(rows, up_ref[deep, :], preferred_element_type=jnp.float32)
    hidden = (silu(gate) * up).astype(jnp.bfloat16)
    term = jnp.dot(hidden, down_ref[...], preferred_element_type=jnp.float32)
    final = pl.num_programs(1) - 1

    @pl.when(step == 0)
    def _():
        total[...] = term

    @pl.when(step > 0)
    def _():
        total[...] += term

    @pl.when(step == final)
    def _():
        for p in range(parts):
            out_ref[p] = total[:, p * depth : (p + 1) * depth].astype(jnp.bfloat16)


def run_experts(rows, gate, up, down):
    parts, experts, count, depth = rows.shape
    width = parts * depth
    units = gate.shape[2]
    tile = min(256, units)
    return pl.pallas_call(
        experts_kernel,
        grid=(experts, units // tile),
        in_specs=[
            pl.BlockSpec((parts, None, count, depth), lambda e, f: (0, e, 0, 0)),
            pl.BlockSpec((None, width, tile), lambda e, f: (e, 0, f)),
            pl.BlockSpec((None, width, tile), lambda e, f: (e, 0, f)),
            pl.BlockSpec((None, tile, width), lambda e, f: (e, f, 0)),
        ],
        out_specs=pl.BlockSpec((parts, None, count, depth), lambda e, f: (0, e, 0, 0)),
        out_shape=jax.ShapeDtypeStruct((parts, experts, count, depth), jnp.bfloat16),
        scratch_shapes=[pltpu.VMEM((count, width), jnp.float32)],
        cost_estimate=pl.CostEstimate(
            flops=6 * experts * count * width * units,
            bytes_accessed=2 * experts * (2 * count * width + 3 * width * units),
            transcendentals=experts * count * units,
        ),
        compiler_params=pltpu.CompilerParams(
            dimension_semantics=("arbitrary", "arbitrary"), vmem_limit_bytes=48 * 1024 * 1024
        ),
        name="experts",
    )(rows, gate, up, down)


def local(
    blender_incoming_features,
    entry_latent_matrix,
    exit_latent_matrix,
    unactivated_valve,
    presoftplus_strides,
    extra_attenuation,
    incoming_feature_kernel,
    entry_latent_kernel,
    exit_latent_kernel,
    stride_offset_vector,
    attenuation_speed_exponent,
    bypass_coef_vector,
    cluster_rescale_coefs,
    blender_result_matrix,
    latter_microbatch_activations,
    specialist_rescale_coefs,
    specialist_valve_matrix,
    specialist_expand_matrix,
    specialist_contract_matrix,
    specialist_picks,
    selected_specialist_coefs,
):
    tap_count = incoming_feature_kernel.shape[0]
    tok_rows = blender_incoming_features.shape[0]
    members_within_cluster = HEADS // SHARING_CLUSTERS
    ep_count = lax.axis_size("ep")
    channels = blender_incoming_features.shape[1]
    latent = entry_latent_matrix.shape[1]
    heads_local = presoftplus_strides.shape[1]
    piece = STATE // ep_count
    tail = tok_rows - HALO
    rim = from_behind(
        jnp.concatenate(
            [
                blender_incoming_features[tail:],
                entry_latent_matrix[tail:],
                exit_latent_matrix[tail:],
            ],
            axis=1,
        ),
        "ep",
        1,
    )
    block_out, conv_c_out, running, pieces = pl.pallas_call(
        functools.partial(ssd_kernel, members_within_cluster),
        in_specs=[VMEM] * 12,
        out_specs=[VMEM] * 4,
        out_shape=[
            jax.ShapeDtypeStruct((tok_rows, channels), jnp.float32),
            jax.ShapeDtypeStruct((tok_rows, latent), jnp.bfloat16),
            jax.ShapeDtypeStruct((tok_rows, heads_local), jnp.float32),
            jax.ShapeDtypeStruct((ep_count, piece + 2, channels), jnp.bfloat16),
        ],
        scratch_shapes=[
            pltpu.VMEM((tok_rows + HALO, members_within_cluster * HEAD_DIM), jnp.float32),
            pltpu.VMEM((STATE, channels), jnp.float32),
        ],
        cost_estimate=pl.CostEstimate(
            flops=2 * tok_rows * tok_rows * channels * 64,
            bytes_accessed=6 * tok_rows * channels * 2,
            transcendentals=tok_rows * tok_rows * heads_local,
        ),
        name="ssd_local",
    )(
        blender_incoming_features,
        entry_latent_matrix,
        exit_latent_matrix,
        rim,
        presoftplus_strides,
        extra_attenuation,
        incoming_feature_kernel,
        entry_latent_kernel,
        exit_latent_kernel,
        stride_offset_vector[None, :],
        attenuation_speed_exponent[None, :],
        bypass_coef_vector[None, :],
    )
    token_count = latter_microbatch_activations.shape[0]
    model_width = latter_microbatch_activations.shape[1]
    local_experts = specialist_valve_matrix.shape[0]
    expert_count = ep_count * local_experts
    capacity = 3 * token_count * TOPK // (2 * expert_count)
    slot_total = expert_count * capacity
    widened = latter_microbatch_activations.astype(jnp.float32)
    share = model_width // lax.axis_size("tp")
    own = lax.axis_index("tp") * share
    normed_b = (
        lax.dynamic_slice_in_dim(latter_microbatch_activations, own, share, 1).astype(jnp.float32)
        * lax.rsqrt(jnp.mean(widened * widened, axis=-1, keepdims=True) + NORM_EPS)
        * lax.dynamic_slice_in_dim(specialist_rescale_coefs, own, share, 0).astype(jnp.float32)
    ).astype(jnp.bfloat16)
    flat_routes = specialist_picks.reshape(-1)
    assigned = flat_routes.shape[0]
    positions = jnp.arange(assigned, dtype=jnp.int32)
    earlier_same = (flat_routes[:, None] == flat_routes[None, :]) & (
        positions[None, :] < positions[:, None]
    )
    slot_rank = jnp.sum(earlier_same.astype(jnp.int32), axis=1)
    slot_of = flat_routes * capacity + slot_rank
    slot_ids = jnp.arange(slot_total, dtype=jnp.int32)
    placing = (slot_ids[:, None] == slot_of[None, :]).astype(jnp.bfloat16)
    placing = jnp.sum(placing.reshape(slot_total, token_count, TOPK), axis=2)
    outgoing = jnp.dot(placing, normed_b, preferred_element_type=jnp.float32).astype(jnp.bfloat16)
    outgoing = outgoing.reshape(ep_count, local_experts, capacity, share)
    chunks = 2 if capacity % 32 == 0 else 1
    size = capacity // chunks
    gathered = []
    for k in range(chunks):
        arrived = lax.all_to_all(
            outgoing[:, :, k * size : (k + 1) * size],
            "ep",
            split_axis=0,
            concat_axis=0,
            tiled=True,
        )
        arrived_rows = arrived.transpose(1, 0, 2, 3).reshape(local_experts, ep_count * size, share)
        gathered.append(lax.all_gather(arrived_rows, "tp"))
    spread = None
    partials = []
    for k in range(chunks):
        if spread is None:
            gathered[k], pieces = lax.optimization_barrier((gathered[k], pieces))
        else:
            gathered[k], spread = lax.optimization_barrier((gathered[k], spread))
        partial_out = run_experts(
            gathered[k],
            specialist_valve_matrix,
            specialist_expand_matrix,
            specialist_contract_matrix,
        )
        if spread is None:
            partial_out, pieces = lax.optimization_barrier((partial_out, pieces))
            spread = lax.all_to_all(pieces, "ep", split_axis=0, concat_axis=0, tiled=True)
        else:
            partial_out, spread = lax.optimization_barrier((partial_out, spread))
        partials.append(partial_out)
    back = []
    for k in range(chunks):
        summed = lax.psum_scatter(partials[k], "tp", scatter_dimension=0, tiled=False)
        summed = summed.reshape(local_experts, ep_count, size, share).transpose(1, 0, 2, 3)
        back.append(lax.all_to_all(summed, "ep", split_axis=0, concat_axis=0, tiled=True))
    returned = back[0] if chunks == 1 else jnp.concatenate(back, axis=2)
    entering = pl.pallas_call(
        prefix_kernel,
        in_specs=[VMEM],
        out_specs=VMEM,
        out_shape=jax.ShapeDtypeStruct((ep_count, piece, channels), jnp.bfloat16),
        name="state_prefix",
    )(spread)
    enter_state = lax.all_to_all(entering, "ep", split_axis=0, concat_axis=0, tiled=True).reshape(
        STATE, channels
    )
    width_a = blender_result_matrix.shape[1]
    tile_a = min(512, width_a)
    whole = lambda *shape: pl.BlockSpec(shape, lambda i: (0,) * len(shape))
    partial_a = pl.pallas_call(
        functools.partial(finish_kernel, members_within_cluster),
        grid=(width_a // tile_a,),
        in_specs=[
            whole(tok_rows, channels),
            whole(tok_rows, latent),
            whole(tok_rows, heads_local),
            whole(STATE, channels),
            whole(tok_rows, channels),
            whole(1, channels),
            pl.BlockSpec((channels, tile_a), lambda i: (0, i)),
        ],
        out_specs=pl.BlockSpec((tok_rows, tile_a), lambda i: (0, i)),
        out_shape=jax.ShapeDtypeStruct((tok_rows, width_a), jnp.bfloat16),
        scratch_shapes=[pltpu.VMEM((tok_rows, channels), jnp.bfloat16)],
        cost_estimate=pl.CostEstimate(
            flops=8 * tok_rows * channels * (width_a + 4 * STATE),
            bytes_accessed=2 * channels * (width_a + 4 * tok_rows) + 2 * tok_rows * width_a,
            transcendentals=2 * tok_rows * channels,
        ),
        compiler_params=pltpu.CompilerParams(dimension_semantics=("arbitrary",)),
        name="finish_mixer",
    )(
        block_out,
        conv_c_out,
        running,
        enter_state,
        unactivated_valve,
        cluster_rescale_coefs[None, :],
        blender_result_matrix,
    )
    tp_count = lax.axis_size("tp")
    terms = lax.all_to_all(
        partial_a.reshape(tp_count, tok_rows // tp_count, width_a),
        "tp",
        split_axis=0,
        concat_axis=0,
        tiled=True,
    )
    mixed_a = jnp.sum(terms.astype(jnp.float32), axis=0).astype(jnp.bfloat16)
    returned = returned.reshape(slot_total, -1)
    token_slots = slot_of.reshape(token_count, TOPK)
    combined = jnp.zeros((token_count, returned.shape[1]), jnp.float32)
    for pick_index in range(TOPK):
        selecting = (token_slots[:, pick_index][:, None] == slot_ids[None, :]).astype(jnp.bfloat16)
        chosen_rows = jnp.dot(selecting, returned, preferred_element_type=jnp.float32)
        combined = combined + chosen_rows * selected_specialist_coefs[:, pick_index][:, None]
    mixed_b = combined.astype(jnp.bfloat16)
    return (mixed_a, mixed_b)


def solution(mesh):
    in_specs = (
        P("ep", "tp"),
        P("ep", "tp"),
        P("ep", "tp"),
        P("ep", "tp"),
        P("ep", "tp"),
        P("ep", "tp"),
        P(None, "tp"),
        P(None, "tp"),
        P(None, "tp"),
        P("tp"),
        P("tp"),
        P("tp"),
        P("tp"),
        P("tp", None),
        P("ep", None),
        P(),
        P("ep", None, "tp"),
        P("ep", None, "tp"),
        P("ep", "tp", None),
        P("ep", None),
        P("ep", None),
    )
    out_specs = (P(("ep", "tp"), None), P("ep", "tp"))
    return jax.shard_map(local, mesh=mesh, in_specs=in_specs, out_specs=out_specs, check_vma=False)
```
